512 devices in a mesh: fs: 64 (over z, y), tp: 8 (over x, core).
Axes of the slice: x: 4, y: 4, z: 16, core: 2. Of those that a mesh axis runs over, the one named last changes fastest.
Arguments:
- saved_inputs: bfloat16 [8192, 4096], P('fs', 'tp'), may hold values from -6 to 6
- value_cotangent: bfloat16 [8192, 2048], P('fs'), may hold values from -0.1875 to 0.1875
- glu_output: bfloat16 [8192, 2048], P('fs', 'tp'), may hold values from -6 to 6
- conv_cotangent: bfloat16 [8192, 2048], P('fs', 'tp'), may hold values from -0.0625 to 0.0625
- factor: bfloat16 [4096, 256], P('tp'), may hold values from -0.09375 to 0.09375
- value_weight: float32 [2048, 4096], P('fs', 'tp'), may hold values from -3 to 3
- first_moment: float32 [2048, 256], P('fs', 'tp'), may hold values from -6 to 6
- second_moment: float32 [2048, 256], P('fs', 'tp'), may hold values from 0.25 to 4
- kernel: float32 [31, 2048], P(None, 'tp'), may hold values from -1 to 1
- kernel_first: float32 [31, 2048], P(None, 'tp'), may hold values from -6 to 6
- kernel_second: float32 [31, 2048], P(None, 'tp'), may hold values from 0.25 to 4
Outputs:
- new_value: float32 [2048, 4096], P('fs', 'tp')
- value_copy: bfloat16 [2048, 4096], P('fs', 'tp')
- value_step: float32 [2048, 4096], P('fs', 'tp')
- new_first: float32 [2048, 256], P('fs', 'tp')
- new_second: float32 [2048, 256], P('fs', 'tp')
- new_kernel: float32 [31, 2048], P(None, 'tp')
- new_kernel_first: float32 [31, 2048], P(None, 'tp')
- new_kernel_second: float32 [31, 2048], P(None, 'tp')
The draws below stay inside these ranges and needn't reach their ends.
All inputs are finite; a program needn't handle non-finite values.
Results may differ from the reference program's by a relative error of at most 0.0055.
Values may be sent and summed in bfloat16 or wider, within the bound.
A program may use at most 64 MiB of HBM per device.

```python
import math
import jax
import jax.numpy as jnp
from jax import lax

WIDTH = 4096
CHANNELS = 2048
TAPS = 31
RANK = 256
TOKENS = 8192


def spiked(entries, own_key, source, target, parts, factor):
    def block_of(axis_at):
        return (jnp.arange(entries.shape[axis_at]) // (entries.shape[axis_at] // parts)).reshape((-1,) + (1,) * (entries.ndim - 1 - axis_at))

    first = jax.random.permutation(own_key, parts)[block_of(target)]
    second = (block_of(target) + parts // 2) % parts
    return jnp.where((block_of(source) == first) | (block_of(source) == second), factor * entries, entries)


def shard_levels(rng, dims, split, least, top_value):
    factor_of, own = 1.0, jax.random.fold_in(rng, 6)
    for position, parts in split:
        heights = jnp.exp(jax.random.uniform(jax.random.fold_in(own, position), (parts,), jnp.float32, least / len(split), top_value / len(split)))
        factor_of = factor_of * jnp.repeat(heights, dims[position] // parts).reshape([-1 if axis == position else 1 for axis in range(len(dims))])
    return factor_of


def noise(stream_key, extent, width, limit, shards=(), kind=jnp.bfloat16):
    drawn = width * jax.random.normal(stream_key, extent, jnp.float32)
    if shards:
        drawn = drawn * shard_levels(stream_key, extent, shards, -0.22, 0.18)
    return jnp.clip(drawn, -limit, limit).astype(kind)


def gaussian_with(rng, extent, width, bound, cuts, heavy, dtype=jnp.bfloat16):
    values = width * jax.random.normal(rng, extent, jnp.float32)
    if cuts:
        values = values * shard_levels(rng, extent, cuts, -0.22, 0.18)
    return jnp.clip(spiked(values, jax.random.fold_in(rng, 3), *heavy), -bound, bound).astype(dtype)


def setup_inputs(seed: int = 0) -> dict:
    arg_keys = jax.random.split(jax.random.key(seed), 12)
    saved_inputs = noise(arg_keys[0], (TOKENS, WIDTH), 1.0, 6.0, ((0, 64), (1, 8)))
    value_cotangent = gaussian_with(arg_keys[1], (TOKENS, CHANNELS), (TOKENS ** -0.5), 0.1875, ((0, 64),), (0, 1, 64, 4.0))
    glu_output = noise(arg_keys[2], (TOKENS, CHANNELS), 1.0, 6.0, ((0, 64), (1, 8)))
    conv_cotangent = noise(arg_keys[3], (TOKENS, CHANNELS), (TOKENS ** -0.5), 0.0625, ((0, 64), (1, 8)))
    factor = noise(arg_keys[4], (WIDTH, RANK), WIDTH ** -0.5, 0.09375, ((0, 8),))
    value_weight = noise(arg_keys[5], (CHANNELS, WIDTH), 0.5, 3.0, ((0, 64), (1, 8)), jnp.float32)
    first_moment = noise(arg_keys[6], (CHANNELS, RANK), 1.0, 6.0, ((0, 64), (1, 8)), jnp.float32)
    second_moment = jnp.clip(jnp.exp(math.log(4.0) - 2.7725887 * jax.random.uniform(arg_keys[7], (CHANNELS, RANK), jnp.float32) ** shard_levels(arg_keys[7], (CHANNELS, RANK), ((0, 64), (1, 8)), -0.2, 0.2)), 0.25, 4.0)
    kernel = noise(arg_keys[8], (TAPS, CHANNELS), TAPS ** -0.5, 1.0, ((1, 8),), jnp.float32)
    kernel_first = noise(arg_keys[9], (TAPS, CHANNELS), 1.0, 6.0, ((1, 8),), jnp.float32)
    kernel_second = jnp.clip(jnp.exp(math.log(4.0) - 2.7725887 * jax.random.uniform(arg_keys[10], (TAPS, CHANNELS), jnp.float32) ** shard_levels(arg_keys[10], (TAPS, CHANNELS), ((1, 8),), -0.2, 0.2)), 0.25, 4.0)
    return {"saved_inputs": saved_inputs, "value_cotangent": value_cotangent, "glu_output": glu_output, "conv_cotangent": conv_cotangent, "factor": factor, "value_weight": value_weight, "first_moment": first_moment, "second_moment": second_moment, "kernel": kernel, "kernel_first": kernel_first, "kernel_second": kernel_second}


def reference(saved_inputs, value_cotangent, glu_output, conv_cotangent, factor, value_weight, first_moment, second_moment, kernel, kernel_first, kernel_second):
    highest = lax.Precision.HIGHEST
    gradient = jnp.dot(value_cotangent.astype(jnp.float32).T, saved_inputs.astype(jnp.float32), precision=highest, preferred_element_type=jnp.float32)
    factor_f = factor.astype(jnp.float32)
    projected = jnp.dot(gradient, factor_f, precision=highest)
    new_first = 0.8 * first_moment + 0.2 * projected
    new_second = 0.9 * second_moment + 0.1 * projected * projected
    direction = new_first / jnp.sqrt(new_second)
    back_proj = jnp.dot(direction, factor_f.T, precision=highest)
    row_mean = lax.optimization_barrier(jnp.mean(back_proj * back_proj, axis=1, keepdims=True))
    value_step = back_proj / jnp.sqrt(row_mean + 0.01)
    new_value = value_weight - 0.05 * value_step
    value_copy = new_value.astype(jnp.bfloat16)
    padded = jnp.pad(glu_output.astype(jnp.float32), ((TAPS - 1, 0), (0, 0)))
    cotangent_f = conv_cotangent.astype(jnp.float32)
    pieces = []
    for offset in range(TAPS):
        begin = TAPS - 1 - offset
        pieces.append(lax.optimization_barrier(jnp.sum(padded[begin:begin + TOKENS] * cotangent_f, axis=0)))
    kernel_grad = jnp.stack(pieces, axis=0)
    new_kernel_first = 0.8 * kernel_first + 0.2 * kernel_grad
    new_kernel_second = 0.9 * kernel_second + 0.1 * kernel_grad * kernel_grad
    new_kernel = kernel - 0.05 * new_kernel_first / jnp.sqrt(new_kernel_second)
    return (new_value, value_copy, value_step, new_first, new_second, new_kernel, new_kernel_first, new_kernel_second)
```

```python
import functools

import jax
import jax.numpy as jnp
from jax import lax
from jax.experimental import pallas as pl
from jax.experimental.pallas import tpu as pltpu
from jax.sharding import PartitionSpec as P

MESH = pl.DeviceIdType.MESH
F32 = jnp.float32
BF16 = jnp.bfloat16
Y = 4
L = 128
HBM = pl.BlockSpec(memory_space=pltpu.HBM)
VM = pl.BlockSpec(memory_space=pltpu.VMEM)
(P1, HALO, GR, GA, CY, CZ, CA, PY, PZ, P3) = range(10)
MM = (((1,), (0,)), ((), ()))
NT = (((1,), (1,)), ((), ()))


def mm(a, b, dims=MM):
    return lax.dot_general(a, b, dims, preferred_element_type=F32)


def split(x):
    upper = x.astype(BF16)
    return upper, (x - upper.astype(F32)).astype(BF16)


def far_first(n):
    return sorted(range(1, n), key=lambda d: -min(d, n - d))


def comm_kernel(
    Z, TP,
    si_h, vc_h, glu_h, cot_h, fac_h, fm_h, sm_h,
    step_o, nf_o, ns_o, kg_o,
    si, vc, glu, cot, fac, fm, sm,
    p1_s, p1_r, halo, ext, acc, lg, cy_r, cz_s, cz_r, ca,
    g_s, g_r, ga, py_s, py_r, pz_s, pz_r, dirs, rhs, ft3, pad, lhs,
    in_sem, send_sem, recv_sem,
):
    f, t = lax.axis_index("fs"), lax.axis_index("tp")
    z, y = f // Y, lax.rem(f, Y)
    FS = Z * Y
    C = 32
    tp_at = lambda d: {"fs": f, "tp": lax.rem(t + d, TP)}
    y_at = lambda d: {"fs": z * Y + lax.rem(y + d, Y), "tp": t}
    z_at = lambda d: {"fs": lax.rem(z + d, Z) * Y + y, "tp": t}
    f_at = lambda d: {"fs": lax.rem(f + d, FS), "tp": t}

    def send(phase, src, dst, where):
        pltpu.make_async_remote_copy(
            src_ref=src, dst_ref=dst, send_sem=send_sem.at[phase], recv_sem=recv_sem.at[phase],
            device_id=where, device_id_type=MESH,
        ).start()

    def take(sem, like):
        pltpu.make_async_copy(like, like, sem).wait()

    def arrived(phase, like):
        take(recv_sem.at[phase], like)

    loads = []
    for i, (src, dst) in enumerate(
        [(si_h, si), (fac_h, fac), (glu_h, glu), (cot_h, cot), (vc_h, vc), (fm_h, fm), (sm_h, sm)]
    ):
        loads.append(pltpu.make_async_copy(src, dst, in_sem.at[i]))
        loads[-1].start()

    barrier = pltpu.get_barrier_semaphore()
    peers = [z_at(d) for d in far_first(Z)]
    peers += [tp_at(d) for d in range(1, TP)] + [y_at(d) for d in range(1, Y)]
    peers += [f_at(1), f_at(FS - 1)]
    for where in peers:
        pl.semaphore_signal(barrier, inc=1, device_id=where, device_id_type=MESH)

    loads[0].wait()
    loads[1].wait()
    partial = mm(si[...], fac[...]).T
    p1_s[...] = partial.astype(BF16).reshape(p1_s.shape)

    tokens = glu.shape[0]
    CB = ext.shape[0]
    loads[2].wait()
    loads[3].wait()
    pl.semaphore_wait(barrier, len(peers))
    for d in range(1, TP):
        to = lax.rem(t + d, TP)
        send(P1, p1_s.at[to], p1_r.at[d - 1], tp_at(d))
    send(HALO, glu.at[pl.ds(tokens - 32, 32)], halo, f_at(1))

    for c in range(CB):
        ext[c, 32:] = glu[:, c * L : (c + 1) * L].astype(F32)
    late = jnp.stack([cot[32:, c * L : (c + 1) * L].astype(F32) for c in range(CB)])
    for k in range(31):
        prod = ext[:, 64 - k : 32 + tokens - k, :] * late
        acc[:, k] = prod.reshape(CB, (tokens - 32) // 8, 8, L).sum(axis=1)

    flip = fac[...].astype(F32).T
    ft3[...] = flip.reshape(ft3.shape)
    width = fac.shape[0]
    ftp = jnp.concatenate([ft3[:, j].reshape(TP * 8, width) for j in range(4)], axis=0).astype(BF16)
    rhs[:, :width] = ftp
    gram = mm(ftp, ftp, NT)
    g_s[...] = gram.reshape(g_s.shape)
    for d in range(1, TP):
        to = lax.rem(t + d, TP)
        send(GR, g_s.at[to], g_r.at[d - 1], tp_at(d))

    arrived(HALO, halo)
    first = (f > 0).astype(F32)
    for c in range(CB):
        ext[c, :32] = halo[:, c * L : (c + 1) * L].astype(F32) * first
    early = jnp.stack([cot[:32, c * L : (c + 1) * L].astype(F32) for c in range(CB)])
    for k in range(31):
        prod = ext[:, 32 - k : 64 - k, :] * early
        acc[:, k] += prod.reshape(CB, 4, 8, L).sum(axis=1)
    acc[:, 31] = jnp.zeros((CB, 8, L), F32)
    for c in range(CB):
        lg[:, :, c * L : (c + 1) * L] = acc[c].sum(axis=1).reshape(4, 8, L)
    for d in range(1, Y):
        to = lax.rem(y + d, Y)
        send(CY, lg.at[to], cy_r.at[d - 1], y_at(d))

    arrived(P1, p1_r)
    reduced = p1_s[t].astype(F32)
    for d in range(1, TP):
        reduced += p1_r[d - 1].astype(F32)
    lhs2 = jnp.concatenate(split(reduced), axis=0)
    loads[4].wait()
    lane = lax.broadcasted_iota(jnp.int32, (16, L), 1)
    left, even = lane < 64, lax.rem(lane, 64) < 32
    for pair in range(Z // 2):
        both = mm(lhs2, vc[:, pair * 2 * L : (pair + 1) * 2 * L])
        both = both[:C] + both[C:]
        v = [
            jnp.concatenate([both[8 * j : 8 * j + 8, :L], both[8 * j : 8 * j + 8, L:]], axis=0)
            for j in range(4)
        ]
        a = [None] * 4
        for j in range(2):
            a[j] = jnp.where(left, v[j], pltpu.roll(v[j + 2], 64, 1))
            a[j + 2] = jnp.where(left, pltpu.roll(v[j], 64, 1), v[j + 2])
        for h in (0, 2):
            py_s[h, pair * 16 : pair * 16 + 16] = jnp.where(
                even, a[h], pltpu.roll(a[h + 1], 32, 1)
            ).astype(BF16)
            py_s[h + 1, pair * 16 : pair * 16 + 16] = jnp.where(
                even, pltpu.roll(a[h], 96, 1), a[h + 1]
            ).astype(BF16)
    for d in range(1, Y):
        to = lax.rem(y + d, Y)
        send(PY, py_s.at[to], py_r.at[d - 1], y_at(d))

    arrived(CY, cy_r)
    taps = lg[y] + cy_r[0] + cy_r[1] + cy_r[2]
    cz_s[...] = taps.astype(BF16)
    for d in far_first(Z):
        send(CZ, cz_s, cz_r.at[d - 1], z_at(d))

    arrived(GR, g_r)
    rows = g_s[t]
    for d in range(1, TP):
        rows += g_r[d - 1]
    ga[t] = rows
    for d in range(1, TP):
        send(GA, ga.at[t], ga.at[t], tp_at(d))

    arrived(PY, py_r)
    summed = py_s[y].astype(F32)
    for d in range(1, Y):
        summed += py_r[d - 1].astype(F32)
    pz_s[...] = summed.reshape(Z, 8, L).astype(BF16)
    for d in far_first(Z):
        to = lax.rem(z + d, Z)
        send(PZ, pz_s.at[to], pz_r.at[d - 1], z_at(d))

    lanes8 = lax.broadcasted_iota(jnp.int32, (8, L), 1)

    def packed(ref):
        pad[...] = jnp.zeros_like(pad)
        pad[:C, :C] = ref[...]
        flipped = pad[...].T
        out = flipped[:8]
        for j in range(1, 4):
            out += pltpu.roll(flipped[8 * j : 8 * j + 8], 32 * j, 1)
        return out

    def unpacked(x):
        for j in range(4):
            pad[8 * j : 8 * j + 8] = x if j == 0 else pltpu.roll(x, L - 32 * j, 1)
        return pad[...].T[:C, :C]

    loads[5].wait()
    loads[6].wait()
    first_moment = packed(fm)
    second_moment = packed(sm)

    arrived(GA, ga.at[pl.ds(0, TP - 1)])
    upper, lower = split(ga[...].reshape(TP * C, TP * C))
    rhs[:, width : width + TP * C] = upper
    rhs[:, width + TP * C :] = lower

    arrived(CZ, cz_r)
    total = taps
    for d in range(1, Z):
        total += cz_r[d - 1].astype(F32)
    ca[y] = total
    for d in range(1, Y):
        send(CA, ca.at[y], ca.at[y], y_at(d))

    arrived(PZ, pz_r)
    projected = pz_s[z].astype(F32)
    for d in range(1, Z):
        projected += pz_r[d - 1].astype(F32)
    new_first = 0.8 * first_moment + 0.2 * projected
    new_second = 0.9 * second_moment + 0.1 * projected * projected
    dirs[t] = new_first / jnp.sqrt(new_second)
    for d in range(1, TP):
        send(P3, dirs.at[t], dirs.at[t], tp_at(d))

    nf_o[...] = unpacked(new_first)
    ns_o[...] = unpacked(new_second)
    arrived(CA, ca.at[pl.ds(0, Y - 1)])
    kg_o[...] = ca[...].reshape(kg_o.shape)
    pad[...] = jnp.zeros_like(pad)

    arrived(P3, dirs.at[pl.ds(0, TP - 1)])
    pad[: TP * 8] = dirs[...].reshape(TP * 8, L)
    by_row = pad[...].T
    blocks = []
    for j in range(4):
        at = j * TP * 8
        piece = by_row[C * j : C * j + C]
        piece = pltpu.roll(piece, at % L, 1) if at % L else piece
        if at // L < len(blocks):
            blocks[-1] = blocks[-1] + piece
        else:
            blocks.append(piece)
    full = jnp.concatenate(blocks, axis=1)[:, : TP * C]
    upper, lower = split(full)
    lhs[:C] = upper
    lhs[C:] = lower
    out = mm(lhs[...], rhs[...])
    back = out[:C, :width] + out[C:, :width]
    lower_at = width + TP * C
    quad = out[:C, width:lower_at] + out[C:, width:lower_at] + out[:C, lower_at:]
    squares = jnp.sum(quad * full, axis=1, keepdims=True)
    mean = jnp.maximum(squares, 0.0) / (width * TP)
    step_o[...] = back / jnp.sqrt(mean + 0.01)

    for phase, like in [
        (P1, p1_r), (HALO, halo), (GR, g_r), (GA, ga.at[pl.ds(0, TP - 1)]), (CY, cy_r), (CZ, cz_r),
        (CA, ca.at[pl.ds(0, Y - 1)]), (PY, py_r), (PZ, pz_r), (P3, dirs.at[pl.ds(0, TP - 1)]),
    ]:
        take(send_sem.at[phase], like)


def final_kernel(
    step, nf, ns, kg, vw, kern, kf, ks,
    new_value, value_copy, value_step, new_first, new_second, new_kernel, new_kf, new_ks,
):
    value_step[...] = step[...]
    value = vw[...] - 0.05 * step[...]
    new_value[...] = value
    value_copy[...] = value.astype(BF16)
    new_first[...] = nf[...]
    new_second[...] = ns[...]
    grad = kg[: kern.shape[0]]
    first = 0.8 * kf[...] + 0.2 * grad
    second = 0.9 * ks[...] + 0.1 * grad * grad
    new_kf[...] = first
    new_ks[...] = second
    new_kernel[...] = kern[...] - 0.05 * first / jnp.sqrt(second)


def body(Z, TP, si, vc, glu, cot, fac, vw, fm, sm, kern, kf, ks):
    width, rank = fac.shape
    tokens, channels = vc.shape
    chans = glu.shape[1]
    CB = chans // L
    shape = jax.ShapeDtypeStruct
    v = pltpu.VMEM
    step, nf, ns, kg = pl.pallas_call(
        functools.partial(comm_kernel, Z, TP),
        out_shape=[
            shape((32, width), F32), shape((32, 32), F32), shape((32, 32), F32), shape((32, chans), F32),
        ],
        in_specs=[HBM] * 7,
        out_specs=[VM] * 4,
        scratch_shapes=[
            v(si.shape, BF16), v(vc.shape, BF16), v(glu.shape, BF16), v(cot.shape, BF16),
            v(fac.shape, BF16), v((32, 32), F32), v((32, 32), F32),
            v((TP, 32, tokens), BF16),
            v((TP - 1, 32, tokens), BF16),
            v((32, chans), BF16),
            v((CB, 32 + tokens, L), F32),
            v((CB, 32, 8, L), F32),
            v((Y, 8, chans), F32),
            v((Y - 1, 8, chans), F32),
            v((8, chans), BF16),
            v((Z - 1, 8, chans), BF16),
            v((Y, 8, chans), F32),
            v((TP, 32, rank), F32),
            v((TP - 1, 32, rank), F32),
            v((TP, 32, rank), F32),
            v((Y, Z * 8, L), BF16),
            v((Y - 1, Z * 8, L), BF16),
            v((Z, 8, L), BF16),
            v((Z - 1, 8, L), BF16),
            v((TP, 8, L), F32),
            v((rank, width + 2 * rank), BF16),
            v((TP, 4, 8, width), F32),
            v((L, L), F32),
            v((64, rank), BF16),
            pltpu.SemaphoreType.DMA((7,)),
            pltpu.SemaphoreType.DMA((10,)),
            pltpu.SemaphoreType.DMA((10,)),
        ],
        compiler_params=pltpu.CompilerParams(
            collective_id=0, has_side_effects=True, vmem_limit_bytes=24 * 1024 * 1024
        ),
        name="comm",
    )(si, vc, glu, cot, fac, fm, sm)
    return pl.pallas_call(
        final_kernel,
        out_shape=[
            shape(vw.shape, F32), shape(vw.shape, BF16), shape(vw.shape, F32),
            shape(fm.shape, F32), shape(fm.shape, F32),
            shape(kern.shape, F32), shape(kern.shape, F32), shape(kern.shape, F32),
        ],
        in_specs=[VM] * 8,
        out_specs=[VM] * 8,
        compiler_params=pltpu.CompilerParams(vmem_limit_bytes=8 * 1024 * 1024),
        name="final",
    )(step, nf, ns, kg, vw, kern, kf, ks)


def solution(mesh):
    placed = (
        P("fs", "tp"), P("fs", None), P("fs", "tp"), P("fs", "tp"), P("tp", None), P("fs", "tp"),
        P("fs", "tp"), P("fs", "tp"), P(None, "tp"), P(None, "tp"), P(None, "tp"),
    )
    return jax.shard_map(
        functools.partial(body, mesh.shape["fs"] // Y, mesh.shape["tp"]),
        mesh=mesh,
        in_specs=placed,
        out_specs=(P("fs", "tp"),) * 5 + (P(None, "tp"),) * 3,
        check_vma=False,
    )
```
